32 devices in a mesh: sp: 8 (over z, y), tp: 4 (over x, core).
Axes of the slice: x: 2, y: 2, z: 4, core: 2. Of those that a mesh axis runs over, the one named last changes fastest.
Arguments:
- resid_in: bfloat16 [2048, 2048], P(('sp', 'tp')), may hold values from -6 to 6
- query_proj: bfloat16 [2048, 512], P('sp', 'tp'), may hold values from -6 to 6
- key_proj: bfloat16 [2048, 256], P('sp', 'tp'), may hold values from -6 to 6
- value_proj: bfloat16 [2048, 256], P('sp', 'tp'), may hold values from -6 to 6
- query_gain: float32 [8, 64], P('tp'), may hold values from 0.5 to 6
- key_gain: float32 [4, 64], P('tp'), may hold values from 0.5 to 6
- out_weight: bfloat16 [512, 2048], replicated, may hold values from -0.25 to 0.25
- norm_gain: float32 [2048], replicated, may hold values from 0.1 to 1.9
- gate_weight: bfloat16 [8, 2048, 1024], P('sp', None, 'tp'), may hold values from -0.125 to 0.125
- up_weight: bfloat16 [8, 2048, 1024], P('sp', None, 'tp'), may hold values from -0.125 to 0.125
- down_weight: bfloat16 [8, 1024, 2048], P('sp', 'tp'), may hold values from -0.1875 to 0.1875
- expert_ids: int32 [2048, 2], P('sp'), may hold values from 0 to 7, all different within a row; in each aligned block of 64 rows (0 to 63, 64 to 127, ...) at most 24 rows name the same one
- route_weight: float32 [2048, 2], P(('sp', 'tp')), may hold values from 0.2 to 1
Outputs:
- layer_out: bfloat16 [2048, 2048], P(('sp', 'tp'))
The draws below stay inside these ranges and needn't reach their ends.
Inputs may be any that keep to these rules, and one draw needn't show every extreme that they name: `expert_ids`: each row names 2 different experts. In each aligned block of rows that one device holds (rows of one index of sp and tp together), no expert is named more than 24 times, and in some blocks one expert is named exactly 24 times.
All inputs are finite; a program needn't handle non-finite values.
Results may differ from the reference program's by a relative error of at most 0.014.
Values may be sent and summed in bfloat16 or wider, within the bound.
A program may use at most 64 MiB of HBM per device.

```python
import math
import jax
import jax.numpy as jnp
import numpy as np
from jax import lax

D = 2048
HEADS = 8
KV_HEADS = 4
HEAD_DIM = 64
FF = 1024
TOPK = 2
GRID_W = 64
TOK_DEV = 256
TOKENS = 2048
EXPERTS = 8
A_WIDTH = 512
FF_DEV = 256
CAP = 24
N_TP = 4


def drawn_pair(key):
    folded = jax.random.fold_in(key, 31)
    query_key, other_key = jax.random.split(folded, 2)
    queries = jnp.clip(jax.random.normal(query_key, (TOKENS, HEADS * HEAD_DIM), jnp.float32), -6.0, 6.0)
    keys_drawn = jnp.clip(jax.random.normal(other_key, (TOKENS, KV_HEADS * HEAD_DIM), jnp.float32), -6.0, 6.0)
    return (queries, keys_drawn)


def draw_query_proj(key, part):
    return drawn_pair(key)[0].astype(jnp.bfloat16)


def draw_key_proj(key, part):
    return drawn_pair(key)[1].astype(jnp.bfloat16)


def gain_table(key, head_count, salt):
    folded = jax.random.fold_in(key, salt)
    first_key = jax.random.fold_in(folded, 0)
    return jax.random.uniform(first_key, (head_count, HEAD_DIM), jnp.float32, 0.5, 2.0)


def draw_query_gain(key, part):
    return gain_table(key, HEADS, 5)


def draw_key_gain(key, part):
    return gain_table(key, KV_HEADS, 9)


def block_scale(stream_key, extent, cuts, smallest, largest):
    factor_of, own = 1.0, jax.random.fold_in(stream_key, 6)
    for position, parts in cuts:
        steps = jnp.exp(jax.random.uniform(jax.random.fold_in(own, position), (parts,), jnp.float32, smallest / len(cuts), largest / len(cuts)))
        factor_of = factor_of * jnp.repeat(steps, extent[position] // parts).reshape([-1 if axis == position else 1 for axis in range(len(extent))])
    return factor_of


def shared_out(own_key, own, number, rows, count, top, most, slope):
    sequence = jax.random.permutation(own_key, count)
    crowded, usual = shares(count, rows * top, most, slope, True), shares(count, rows * top, most, slope, False)
    places = jnp.arange(count)

    def named(tallies, rotation):
        used = int((tallies > 0).sum())
        fixed = max(1, used // 4)
        passed = fixed + (places - fixed + rotation * (used - fixed)) % max(1, count - fixed)
        return jnp.zeros((count,), jnp.int32).at[sequence[jnp.where(places < fixed, places, passed)]].set(jnp.asarray(tallies, jnp.int32))

    tallies = jnp.where(number % 4 == 0, named(crowded, number // 4), named(usual, number - number // 4 - 1))
    mixed = jax.random.permutation(jax.random.fold_in(own, 3), count)
    giver, taker = mixed[0:count // 2 * 2:2], mixed[1:count // 2 * 2:2]
    margin = jnp.minimum(tallies[giver] - 1, most - tallies[taker]) // 2
    margin = jnp.where((giver == sequence[0]) | (taker == sequence[0]) | (tallies[taker] == 0), 0, jnp.maximum(margin, 0))
    passed = jax.random.randint(jax.random.fold_in(own, 4), (count // 2,), 0, 1 << 20) % (margin + 1)
    tallies = tallies.at[giver].add(-passed).at[taker].add(passed)
    items = jnp.searchsorted(jnp.cumsum(tallies), jnp.arange(rows * top), side="right").astype(jnp.int32)
    table = items.reshape(top, rows).T
    table = table[jax.random.permutation(jax.random.fold_in(own, 1), rows)]
    rotation = jax.random.randint(jax.random.fold_in(own, 2), (rows, 1), 0, top)
    return jnp.take_along_axis(table, (jnp.arange(top)[None, :] + rotation) % top, axis=1)


def shares(count, total, bound, slope, full):
    portions = [(1 << 20) // math.isqrt(standing ** slope) + 1 for standing in range(1, count + 1)]
    largest = bound if full else min(bound, max(-(-total // count), total * portions[0] // sum(portions)))
    least = 1 if total - largest >= count - 1 else 0
    holding, surplus = [largest] + [least] * (count - 1), total - largest - least * (count - 1)
    while surplus > 0:
        candidates = [i for i in range(1, count) if holding[i] < largest] or [i for i in range(1, count) if holding[i] < bound]
        mass, budget = sum([portions[i] for i in candidates]), surplus
        for i in candidates:
            addition = min(bound - holding[i], max(1, budget * portions[i] // mass), surplus)
            holding[i] = holding[i] + addition
            surplus = surplus - addition
    return np.array(holding)


def centred(own_key, shape, deviation, limit, cuts=(), kind=jnp.bfloat16):
    array = jax.random.normal(own_key, shape, jnp.float32) * deviation
    if len(cuts) > 0:
        array = block_scale(own_key, shape, cuts, -0.22, 0.18) * array
    return jnp.clip(array, min=-limit, max=limit).astype(kind)


def setup_inputs(seed: int = 0) -> dict:
    key_of = jax.random.split(jax.random.key(seed), 14)
    resid_in = centred(key_of[0], (TOKENS, D), 1.0, 6.0, ((0, 32),))
    query_proj = draw_query_proj(jax.random.fold_in(key_of[13], 71), 0)
    key_proj = draw_key_proj(jax.random.fold_in(key_of[13], 71), 0)
    value_proj = centred(key_of[3], (TOKENS, KV_HEADS * HEAD_DIM), 1.0, 6.0, ((0, 8), (1, 4)))
    query_gain = draw_query_gain(jax.random.fold_in(key_of[13], 71), 0)
    key_gain = draw_key_gain(jax.random.fold_in(key_of[13], 71), 0)
    out_weight = centred(key_of[6], (A_WIDTH, D), A_WIDTH ** -0.5, 0.25)
    norm_gain = jnp.clip(1.0 + 0.18 * jax.random.normal(key_of[7], (D,), jnp.float32), 0.1, 1.9)
    gate_weight = centred(key_of[8], (EXPERTS, D, FF), D ** -0.5, 0.125, ((0, 8), (2, 4)))
    up_weight = centred(key_of[9], (EXPERTS, D, FF), D ** -0.5, 0.125, ((0, 8), (2, 4)))
    down_weight = centred(key_of[10], (EXPERTS, FF, D), FF ** -0.5, 0.1875, ((0, 8), (1, 4)))
    expert_ids_keys = jax.random.split(jax.random.fold_in(key_of[11], 1), TOKENS // (TOK_DEV // N_TP))
    expert_ids_turns = jax.random.permutation(jax.random.fold_in(key_of[11], 3), TOKENS // (TOK_DEV // N_TP))
    expert_ids = jax.vmap(lambda own, number: shared_out(jax.random.fold_in(key_of[11], 2), own, number, TOK_DEV // N_TP, EXPERTS, TOPK, CAP, 1))(expert_ids_keys, expert_ids_turns).reshape((TOKENS, TOPK))
    route_weight = jnp.clip(0.2 + 0.8 * jax.random.uniform(key_of[12], (TOKENS, TOPK), jnp.float32) ** block_scale(key_of[12], (TOKENS, TOPK), ((0, 32),), -0.2, 0.2), 0.2, 1.0)
    return {"resid_in": resid_in, "query_proj": query_proj, "key_proj": key_proj, "value_proj": value_proj, "query_gain": query_gain, "key_gain": key_gain, "out_weight": out_weight, "norm_gain": norm_gain, "gate_weight": gate_weight, "up_weight": up_weight, "down_weight": down_weight, "expert_ids": expert_ids, "route_weight": route_weight}


eps = 1e-06
rope_base = 10000.0
query_block = 64

def rotary_tables(positions):
    row_pos = (positions // GRID_W).astype(jnp.float32)
    col_pos = (positions % GRID_W).astype(jnp.float32)
    freq_count = HEAD_DIM // 4
    inverse = rope_base ** (-jnp.arange(freq_count, dtype=jnp.float32) / freq_count)
    angles = jnp.concatenate([row_pos[:, None] * inverse, col_pos[:, None] * inverse], axis=-1)
    return (jnp.cos(angles), jnp.sin(angles))

def prepare(projected, gains, cosine, sine_table):
    tok_total = projected.shape[0]
    head_count = gains.shape[0]
    values_f = projected.astype(jnp.float32).reshape(tok_total, head_count, HEAD_DIM)
    normed = values_f * lax.rsqrt(lax.optimization_barrier(jnp.mean(values_f * values_f, axis=-1, keepdims=True)) + eps) * gains[None]
    half_dim = HEAD_DIM // 2
    first_half = normed[..., :half_dim]
    second_half = normed[..., half_dim:]
    cos_b = cosine[:, None, :]
    sin_b = sine_table[:, None, :]
    rotated = jnp.concatenate([first_half * cos_b - second_half * sin_b, second_half * cos_b + first_half * sin_b], axis=-1)
    return rotated.astype(jnp.bfloat16)

def reference(resid_in, query_proj, key_proj, value_proj, query_gain, key_gain, out_weight, norm_gain, gate_weight, up_weight, down_weight, expert_ids, route_weight):
    positions = jnp.arange(TOKENS, dtype=jnp.int32)
    cosine, sine_table = rotary_tables(positions)
    query_rot = prepare(query_proj, query_gain, cosine, sine_table)
    key_rot = prepare(key_proj, key_gain, cosine, sine_table)
    group_size = HEADS // KV_HEADS
    grouped = query_rot.reshape(TOKENS // query_block, query_block, KV_HEADS, group_size, HEAD_DIM)
    key_f = key_rot.astype(jnp.float32)
    value_f = value_proj.reshape(TOKENS, KV_HEADS, HEAD_DIM).astype(jnp.float32)

    def attend_block(block_q):
        scores = jnp.einsum('qkgd,skd->qkgs', block_q.astype(jnp.float32), key_f) * HEAD_DIM ** (-0.5)
        row_max = lax.optimization_barrier(jnp.max(scores, axis=-1, keepdims=True))
        exponents = jnp.exp(scores - row_max)
        weights = exponents.astype(jnp.bfloat16)
        row_sum = lax.optimization_barrier(jnp.sum(exponents, axis=-1))
        summed_values = jnp.einsum('qkgs,skd->qkgd', weights.astype(jnp.float32), value_f)
        return (summed_values / row_sum[..., None]).astype(jnp.bfloat16)
    attended = lax.map(attend_block, grouped).reshape(TOKENS, HEADS * HEAD_DIM)
    mixed_out = jnp.dot(attended, out_weight, preferred_element_type=jnp.float32)
    residual = (resid_in.astype(jnp.float32) + mixed_out).astype(jnp.bfloat16)
    resid_f = residual.astype(jnp.float32)
    normed = (resid_f * lax.rsqrt(lax.optimization_barrier(jnp.mean(resid_f * resid_f, axis=-1, keepdims=True)) + eps) * norm_gain).astype(jnp.bfloat16)
    block_rows = TOK_DEV // N_TP
    n_blocks = TOKENS // block_rows
    ids_blocks = expert_ids.reshape(n_blocks, block_rows * TOPK).astype(jnp.int32)
    member = (ids_blocks[:, :, None] == jnp.arange(EXPERTS, dtype=jnp.int32)[None, None, :]).astype(jnp.int32)
    ranks = lax.optimization_barrier(jnp.sum((jnp.cumsum(member, axis=1) - member) * member, axis=2))
    block_index = jnp.arange(n_blocks, dtype=jnp.int32)[:, None]
    slot_pos = (block_index * CAP + ranks).astype(jnp.int32)
    token_of = jnp.repeat(jnp.arange(TOKENS, dtype=jnp.int32), TOPK).reshape(n_blocks, block_rows * TOPK)
    row_table = jnp.full((EXPERTS, n_blocks * CAP), TOKENS, jnp.int32).at[ids_blocks, slot_pos].set(token_of)
    normed_pad = jnp.concatenate([normed, jnp.zeros((1, D), jnp.bfloat16)], axis=0)

    def run_expert(args):
        table_row, gate_e, up_e, down_e = args
        rows = normed_pad[table_row]
        gate = jnp.dot(rows, gate_e, preferred_element_type=jnp.float32)
        upper = jnp.dot(rows, up_e, preferred_element_type=jnp.float32)
        hidden = (jax.nn.silu(gate) * upper).astype(jnp.bfloat16)
        accum = jnp.zeros((rows.shape[0], D), jnp.float32)
        for block_index_ff in range(FF // FF_DEV):
            lower = block_index_ff * FF_DEV
            partial_value = jnp.dot(hidden[:, lower:lower + FF_DEV], down_e[lower:lower + FF_DEV], preferred_element_type=jnp.float32)
            accum = accum + lax.optimization_barrier(partial_value.astype(jnp.bfloat16)).astype(jnp.float32)
        return accum.astype(jnp.bfloat16)
    outputs_all = lax.map(run_expert, (row_table, gate_weight, up_weight, down_weight))
    picked = outputs_all[ids_blocks, slot_pos].reshape(TOKENS, TOPK, D).astype(jnp.float32)
    combined = lax.optimization_barrier(jnp.sum(picked * route_weight[:, :, None], axis=1))
    return (resid_f + combined).astype(jnp.bfloat16)
```

```python
import functools

import jax
import jax.numpy as jnp
import numpy as np
from jax import lax
from jax.experimental import pallas as pl
from jax.experimental.pallas import tpu as pltpu
from jax.sharding import PartitionSpec as P

HEAD_DIM = 64
TOPK = 2
GRID_W = 64
TOK_DEV = 256
LANES = 128

eps = 1e-06
rope_base = 10000.0

BF = jnp.bfloat16
F32 = jnp.float32
MESH = pl.DeviceIdType.MESH


def rotary_table(tokens):
    positions = np.arange(tokens)
    freq_count = HEAD_DIM // 4
    inverse = (rope_base ** (-np.arange(freq_count, dtype=np.float32) / freq_count)).astype(np.float32)
    row_pos = (positions // GRID_W).astype(np.float32)
    col_pos = (positions % GRID_W).astype(np.float32)
    angles = np.concatenate([row_pos[:, None] * inverse, col_pos[:, None] * inverse], axis=-1)
    angles = angles.astype(np.float32)
    return np.concatenate([np.cos(angles), np.sin(angles)], axis=-1).astype(np.float32)


def lane_of(shape):
    return lax.broadcasted_iota(jnp.int32, shape, 1)


def prepare(x, gain, cos4, sin4):
    lane = lane_of(x.shape)
    low = lane < HEAD_DIM
    sq = x * x
    s_low = jnp.sum(jnp.where(low, sq, 0.0), axis=-1, keepdims=True) / HEAD_DIM
    s_high = jnp.sum(jnp.where(low, 0.0, sq), axis=-1, keepdims=True) / HEAD_DIM
    y = x * jnp.where(low, lax.rsqrt(s_low + eps), lax.rsqrt(s_high + eps)) * gain
    half = HEAD_DIM // 2
    first = (lane % HEAD_DIM) < half
    swapped = jnp.where(first, pltpu.roll(y, LANES - half, 1), pltpu.roll(y, half, 1))
    return y * cos4 + swapped * sin4


def kernel(
    n, cap, groups,
    resid_h, q_ref, k_ref, v_ref, qg_ref, kg_ref, ow_h, ng_ref, gw_h, uw_h, dw_h, ids_ref, rw_ref, tab_h,
    out_ref,
    resid, ow, gw, uw, dw, tab, kv, qx, mx, acc, att, attg, res_f, send, rows, hid, hidg, back, ret,
    loc, kv_ss, kv_rs, kf_ss, kf_rs, at_ss, at_rs, dw_ss, dw_rs, a_ss, a_rs, x_ss, x_rs,
    s_ss, s_rs, o_ss, o_rs, h_ss, h_rs, r_ss, r_rs,
):
    tok = q_ref.shape[0]
    tp = 4
    rown = tok // tp
    width = out_ref.shape[1]
    per = n // groups
    half_n = n // 2
    e = lax.axis_index("sp")
    j = lax.axis_index("tp")
    jx, jc = j // 2, j % 2
    xp = (1 - jx) * 2 + jc
    sib = jx * 2 + (1 - jc)
    a, b = e // 2, e % 2
    ypart = a * 2 + (1 - b)

    def rcopy(src, dst, ss, rs, s_id, t_id):
        return pltpu.make_async_remote_copy(
            src_ref=src, dst_ref=dst, send_sem=ss, recv_sem=rs,
            device_id=(s_id, t_id), device_id_type=MESH,
        )

    locals_ = [
        pltpu.make_async_copy(tab_h.at[pl.ds(e * tok, tok)], tab, loc.at[0]),
        pltpu.make_async_copy(dw_h.at[0], dw.at[j], loc.at[1]),
        pltpu.make_async_copy(ow_h, ow, loc.at[2]),
        pltpu.make_async_copy(resid_h, resid, loc.at[3]),
        pltpu.make_async_copy(gw_h.at[0], gw, loc.at[4]),
        pltpu.make_async_copy(uw_h.at[0], uw, loc.at[5]),
    ]
    for c in locals_:
        c.start()

    barrier = pltpu.get_barrier_semaphore()

    def greet(k, carry):
        pl.semaphore_signal(barrier, inc=1, device_id=(lax.rem(e + k, n), j), device_id_type=MESH)
        return carry

    lax.fori_loop(1, n, greet, 0)
    for k in range(1, tp):
        pl.semaphore_signal(barrier, inc=1, device_id=(e, lax.rem(j + k, tp)), device_id_type=MESH)

    locals_[0].wait()
    cs = tab[:, : HEAD_DIM // 2]
    sn = tab[:, HEAD_DIM // 2 :]
    cos4 = jnp.concatenate([cs, cs, cs, cs], axis=1)
    sin4 = jnp.concatenate([-sn, sn, -sn, sn], axis=1)
    k_in = k_ref[...].astype(F32)
    v_in = v_ref[...].astype(F32)
    low = lane_of((tok, LANES)) < HEAD_DIM
    kv_in = jnp.concatenate([k_in, v_in], axis=1)
    kgain = jnp.concatenate([kg_ref[...], kg_ref[...]], axis=1)
    kv[e] = jnp.where(low, prepare(kv_in, kgain, cos4, sin4), kv_in).astype(BF)
    pl.semaphore_wait(barrier, n - 1 + tp - 1)

    def kv_send(d):
        to = lax.rem(a + d, half_n) * 2 + b
        return rcopy(kv.at[e], kv.at[e], kv_ss.at[d], kv_rs.at[d], to, j)

    def kv_recv(d):
        src = lax.rem(a + half_n - d, half_n) * 2 + b
        return rcopy(kv.at[src], kv.at[src], kv_ss.at[d], kv_rs.at[d], e, j)

    def kf_send(d):
        src = lax.rem(a + half_n - d, half_n) * 2 + b
        return rcopy(kv.at[src], kv.at[src], kf_ss.at[d], kf_rs.at[d], ypart, j)

    def kf_recv(d):
        src = lax.rem(a + half_n - d, half_n) * 2 + (1 - b)
        return rcopy(kv.at[src], kv.at[src], kf_ss.at[d], kf_rs.at[d], ypart, j)

    def loop(lo, hi, fn):
        def step(i, carry):
            fn(i)
            return carry
        lax.fori_loop(lo, hi, step, 0)

    loop(1, half_n, lambda d: kv_send(d).start())
    kf_send(0).start()

    locals_[1].wait()
    dw_x = rcopy(dw.at[j], dw.at[j], dw_ss.at[0], dw_rs.at[0], e, xp)
    dw_s = rcopy(dw.at[j], dw.at[j], dw_ss.at[1], dw_rs.at[1], e, sib)
    dw_o = rcopy(dw.at[xp], dw.at[xp], dw_ss.at[2], dw_rs.at[2], e, sib)
    dw_x.start()
    dw_s.start()

    qgain = jnp.concatenate([qg_ref[0:1, :], qg_ref[1:2, :]], axis=1)
    q = prepare(q_ref[...].astype(F32), qgain, cos4, sin4) * (HEAD_DIM**-0.5)
    qx[0:tok] = jnp.where(low, q, 0.0).astype(BF)
    qx[tok : 2 * tok] = jnp.where(low, pltpu.roll(q, HEAD_DIM, 1), 0.0).astype(BF)
    mx[...] = jnp.full(mx.shape, -jnp.inf, F32)
    acc[...] = jnp.zeros(acc.shape, F32)

    def attend(d):
        @pl.when(d > 0)
        def _():
            kv_recv(d).wait_recv()
            kf_send(d).start()

        kf_recv(d).wait_recv()
        base = lax.rem(a + half_n - d, half_n) * 2
        keys = jnp.concatenate([kv[base], kv[base + 1]], axis=0)
        vals = jnp.where(lane_of(keys.shape) < HEAD_DIM, jnp.ones_like(keys), keys)
        for blk in range(4):
            rs = pl.ds(blk * (2 * tok // 4), 2 * tok // 4)
            sc = lax.dot_general(qx[rs], keys, (((1,), (1,)), ((), ())), preferred_element_type=F32)
            old = mx[rs]
            new = jnp.maximum(old, jnp.max(sc, axis=-1, keepdims=True))
            p = jnp.exp(sc - new[:, 0:1])
            mx[rs] = new
            acc[rs] = acc[rs] * jnp.exp(old - new) + jnp.dot(p.astype(BF), vals, preferred_element_type=F32)

    loop(0, half_n, attend)
    o = acc[...]
    o = o / pltpu.roll(o, HEAD_DIM, 1)
    att[...] = jnp.where(low, pltpu.roll(o[0:tok], HEAD_DIM, 1), o[tok : 2 * tok]).astype(BF)

    def at_copy(k):
        to = lax.rem(j + k, tp)
        return rcopy(att.at[pl.ds(to * rown, rown)], attg.at[j], at_ss.at[k], at_rs.at[k], e, to)

    def at_recv(k):
        src = lax.rem(j + tp - k, tp)
        return rcopy(att.at[pl.ds(0, rown)], attg.at[src], at_ss.at[k], at_rs.at[k], e, src)

    for k in range(1, tp):
        at_copy(k).start()
    attg[j] = att[pl.ds(j * rown, rown), :]

    slots = n * cap
    ids = ids_ref[pl.ds(j * rown, rown), :]
    rw = rw_ref[...]
    col = lax.broadcasted_iota(jnp.int32, (rown, slots), 1)
    off0 = col - ids[:, 0:1] * cap
    off1 = col - ids[:, 1:2] * cap
    in0 = (off0 >= 0) & (off0 < cap)
    in1 = (off1 >= 0) & (off1 < cap)
    member = jnp.where(in0 | in1, 1.0, 0.0)
    ti = lax.broadcasted_iota(jnp.int32, (rown, rown), 0)
    tj = lax.broadcasted_iota(jnp.int32, (rown, rown), 1)
    before = jnp.where(tj < ti, 1.0, 0.0)
    rank = jnp.dot(before.astype(BF), member.astype(BF), preferred_element_type=F32)
    offset = jnp.where(in0, off0, off1).astype(F32)
    hit = jnp.where(rank == offset, member, 0.0)
    weight = hit * jnp.where(in0, rw[:, 0:1], rw[:, 1:2])

    locals_[2].wait()
    locals_[3].wait()
    for k in range(1, tp):
        at_recv(k).wait_recv()
    joined = jnp.concatenate([attg[i] for i in range(tp)], axis=1)
    mixed = jnp.dot(joined, ow[...], preferred_element_type=F32)
    residual = (resid[...].astype(F32) + mixed).astype(BF).astype(F32)
    res_f[...] = residual
    scale = lax.rsqrt(jnp.mean(residual * residual, axis=-1, keepdims=True) + eps)
    normed = (residual * scale * ng_ref[...]).astype(BF)
    out_rows = lax.dot_general(
        hit.astype(BF), normed, (((0,), (0,)), ((), ())), preferred_element_type=F32
    )
    send[...] = out_rows.reshape(n, cap, width).astype(BF)

    def a_send(k):
        to = lax.rem(e + k, n)
        return rcopy(send.at[to], rows.at[j, k], a_ss.at[k], a_rs.at[k], to, j)

    def a_recv(k):
        return rcopy(send.at[0], rows.at[j, k], a_ss.at[k], a_rs.at[k], e, j)

    loop(1, n, lambda k: a_send(k).start())
    rows[j, 0] = send[e]
    dw_x_in = rcopy(dw.at[xp], dw.at[xp], dw_ss.at[0], dw_rs.at[0], e, xp)
    dw_x_in.wait_recv()
    dw_o.start()
    locals_[4].wait()
    locals_[5].wait()

    def part(t, g):
        return rows.at[t, pl.ds(g * per, per)]

    def x_send(g):
        return rcopy(part(j, g), part(j, g), x_ss.at[g], x_rs.at[g], e, xp)

    def x_recv(g):
        return rcopy(part(xp, g), part(xp, g), x_ss.at[g], x_rs.at[g], e, xp)

    def s_send(g):
        return rcopy(part(j, g), part(j, g), s_ss.at[g], s_rs.at[g], e, sib)

    def s_recv(g):
        return rcopy(part(sib, g), part(sib, g), s_ss.at[g], s_rs.at[g], e, sib)

    def o_send(g):
        return rcopy(part(xp, g), part(xp, g), o_ss.at[g], o_rs.at[g], e, sib)

    dg = (1 - jx) * 2 + (1 - jc)

    def o_recv(g):
        return rcopy(part(dg, g), part(dg, g), o_ss.at[g], o_rs.at[g], e, sib)

    def h_send(g, k):
        to = lax.rem(j + k, tp)
        return rcopy(hid.at[g, to], hidg.at[g, j], h_ss.at[g, k], h_rs.at[g, k], e, to)

    def h_recv(g, k):
        src = lax.rem(j + tp - k, tp)
        return rcopy(hid.at[g, 0], hidg.at[g, src], h_ss.at[g, k], h_rs.at[g, k], e, src)

    def r_send(k):
        to = lax.rem(e + n - k, n)
        return rcopy(back.at[k], ret.at[e], r_ss.at[k], r_rs.at[k], to, j)

    def r_recv(k):
        src = lax.rem(e + k, n)
        return rcopy(back.at[k], ret.at[src], r_ss.at[k], r_rs.at[k], e, j)

    m = per * cap

    def stage_a(g):
        def one(i):
            k = g * per + i

            @pl.when(k > 0)
            def _():
                a_recv(k).wait_recv()

        loop(0, per, one)
        x_send(g).start()
        s_send(g).start()

    def stage_c(g):
        x_recv(g).wait_recv()
        o_send(g).start()
        s_recv(g).wait_recv()
        o_recv(g).wait_recv()
        block = rows[:, pl.ds(g * per, per)].astype(F32).reshape(tp * m, width).astype(BF)
        gate = jnp.dot(block, gw[...], preferred_element_type=F32)
        upper = jnp.dot(block, uw[...], preferred_element_type=F32)
        hidden = gate / (1.0 + jnp.exp(-gate)) * upper
        hid[g] = hidden.reshape(tp, m, hidden.shape[1]).astype(BF)
        for k in range(1, tp):
            h_send(g, k).start()
        hidg[g, j] = hid[g, j]

    def stage_d(g):
        for k in range(1, tp):
            h_recv(g, k).wait_recv()

        @pl.when(g == 0)
        def _():
            rcopy(dw.at[sib], dw.at[sib], dw_ss.at[1], dw_rs.at[1], e, sib).wait_recv()
            rcopy(dw.at[dg], dw.at[dg], dw_ss.at[2], dw_rs.at[2], e, sib).wait_recv()

        joined_h = jnp.concatenate([hidg[g, i] for i in range(tp)], axis=1)
        cols = 512

        def column(ci):
            cd = pl.ds(pl.multiple_of(ci * cols, cols), cols)
            dfull = dw[:, :, cd].reshape(joined_h.shape[1], cols)
            y = jnp.dot(joined_h, dfull, preferred_element_type=F32)
            back[pl.ds(g * per, per), :, cd] = y.reshape(per, cap, cols).astype(BF)

        for ci in range(width // cols):
            column(ci)

        def one(i):
            k = g * per + i

            @pl.when(k > 0)
            def _():
                r_send(k).start()

        loop(0, per, one)

    def tick(t):
        @pl.when(t < groups)
        def _():
            stage_a(t)

        @pl.when(t >= 2)
        def _():
            stage_d(t - 2)

        @pl.when((t >= 1) & (t <= groups))
        def _():
            stage_c(t - 1)

    loop(0, groups + 2, tick)
    ret[e] = back[0]
    loop(1, n, lambda k: r_recv(k).wait_recv())
    w_hi = weight.astype(BF)
    w_lo = (weight - w_hi.astype(F32)).astype(BF)
    back_rows = ret[...].astype(F32).reshape(slots, width).astype(BF)
    total = jnp.dot(w_hi, back_rows, preferred_element_type=F32)
    total += jnp.dot(w_lo, back_rows, preferred_element_type=F32)
    out_ref[...] = (res_f[...] + total).astype(BF)

    def drain(k):
        a_send(k).wait_send()
        r_send(k).wait_send()

    loop(1, n, drain)
    loop(1, half_n, lambda d: kv_send(d).wait_send())
    loop(0, half_n, lambda d: kf_send(d).wait_send())
    for k in range(1, tp):
        at_copy(k).wait_send()
    dw_x.wait_send()
    dw_s.wait_send()
    dw_o.wait_send()

    def drain_g(g):
        x_send(g).wait_send()
        s_send(g).wait_send()
        o_send(g).wait_send()
        for k in range(1, tp):
            h_send(g, k).wait_send()

    loop(0, groups, drain_g)


def body(resid_in, query_proj, key_proj, value_proj, query_gain, key_gain, out_weight, norm_gain,
         gate_weight, up_weight, down_weight, expert_ids, route_weight):
    n = lax.axis_size("sp")
    tp = lax.axis_size("tp")
    tok = query_proj.shape[0]
    rown = tok // tp
    width = resid_in.shape[1]
    ff = gate_weight.shape[2]
    need = max(2, 3 * TOPK * TOK_DEV // (2 * tp * n))
    cap = -(-need // 8) * 8
    groups = 4
    per = n // groups
    table = jnp.asarray(rotary_table(n * tok))
    vm = pl.BlockSpec(memory_space=pltpu.VMEM)
    hb = pl.BlockSpec(memory_space=pl.ANY)
    dma = pltpu.SemaphoreType.DMA
    V = pltpu.VMEM
    scratch = [
        V((rown, width), BF),
        V(out_weight.shape, BF),
        V((width, ff), BF),
        V((width, ff), BF),
        V((tp, ff, width), BF),
        V((tok, HEAD_DIM), F32),
        V((n, tok, LANES), BF),
        V((2 * tok, LANES), BF),
        V((2 * tok, LANES), F32),
        V((2 * tok, LANES), F32),
        V((tok, LANES), BF),
        V((tp, rown, LANES), BF),
        V((rown, width), F32),
        V((n, cap, width), BF),
        V((tp, n, cap, width), BF),
        V((groups, tp, per * cap, ff), BF),
        V((groups, tp, per * cap, ff), BF),
        V((n, cap, width), BF),
        V((n, cap, width), BF),
        dma((6,)),
        dma((n // 2,)), dma((n // 2,)), dma((n // 2,)), dma((n // 2,)),
        dma((tp,)), dma((tp,)), dma((3,)), dma((3,)),
        dma((n,)), dma((n,)),
        dma((groups,)), dma((groups,)), dma((groups,)), dma((groups,)), dma((groups,)), dma((groups,)),
        dma((groups, tp)), dma((groups, tp)),
        dma((n,)), dma((n,)),
    ]
    return pl.pallas_call(
        functools.partial(kernel, n, cap, groups),
        out_shape=jax.ShapeDtypeStruct((rown, width), BF),
        in_specs=[hb, vm, vm, vm, vm, vm, hb, vm, hb, hb, hb, vm, vm, hb],
        out_specs=vm,
        scratch_shapes=scratch,
        compiler_params=pltpu.CompilerParams(
            collective_id=0, has_side_effects=True, vmem_limit_bytes=60 * 1024 * 1024
        ),
    )(resid_in, query_proj, key_proj, value_proj, query_gain, key_gain, out_weight,
      norm_gain.reshape(1, width), gate_weight, up_weight, down_weight, expert_ids, route_weight, table)


def solution(mesh):
    placed = (
        P(("sp", "tp"), None),
        P("sp", "tp"),
        P("sp", "tp"),
        P("sp", "tp"),
        P("tp", None),
        P("tp", None),
        P(),
        P(),
        P("sp", None, "tp"),
        P("sp", None, "tp"),
        P("sp", "tp", None),
        P("sp", None),
        P(("sp", "tp"), None),
    )
    return jax.shard_map(
        body, mesh=mesh, in_specs=placed, out_specs=P(("sp", "tp"), None), check_vma=False
    )
```

```python
import functools

import jax
import jax.numpy as jnp
import numpy as np
from jax import lax
from jax.experimental import pallas as pl
from jax.experimental.pallas import tpu as pltpu
from jax.sharding import PartitionSpec as P

HEAD_DIM = 64
TOPK = 2
GRID_W = 64
TOK_DEV = 256
LANES = 128

eps = 1e-06
rope_base = 10000.0

BF = jnp.bfloat16
F32 = jnp.float32
MESH = pl.DeviceIdType.MESH


def rotary_table(tokens):
    positions = np.arange(tokens)
    freq_count = HEAD_DIM // 4
    inverse = (rope_base ** (-np.arange(freq_count, dtype=np.float32) / freq_count)).astype(np.float32)
    row_pos = (positions // GRID_W).astype(np.float32)
    col_pos = (positions % GRID_W).astype(np.float32)
    angles = np.concatenate([row_pos[:, None] * inverse, col_pos[:, None] * inverse], axis=-1)
    angles = angles.astype(np.float32)
    return np.concatenate([np.cos(angles), np.sin(angles)], axis=-1).astype(np.float32)


def lane_of(shape):
    return lax.broadcasted_iota(jnp.int32, shape, 1)


def prepare(x, gain, cos4, sin4):
    lane = lane_of(x.shape)
    low = lane < HEAD_DIM
    sq = x * x
    s_low = jnp.sum(jnp.where(low, sq, 0.0), axis=-1, keepdims=True) / HEAD_DIM
    s_high = jnp.sum(jnp.where(low, 0.0, sq), axis=-1, keepdims=True) / HEAD_DIM
    y = x * jnp.where(low, lax.rsqrt(s_low + eps), lax.rsqrt(s_high + eps)) * gain
    half = HEAD_DIM // 2
    first = (lane % HEAD_DIM) < half
    swapped = jnp.where(first, pltpu.roll(y, LANES - half, 1), pltpu.roll(y, half, 1))
    return y * cos4 + swapped * sin4


def kernel(
    n, cap, groups,
    resid_h, q_ref, k_ref, v_ref, qg_ref, kg_ref, ow_h, ng_ref, gw_h, uw_h, dw_h, ids_ref, rw_ref, tab_h,
    out_ref,
    resid, ow, gw, uw, dw, tab, kv, qx, mx, acc, att, attg, res_f, send, rows, hid, hidg, back, ret, ids_t,
    loc, kv_ss, kv_rs, kf_ss, kf_rs, at_ss, at_rs, dw_ss, dw_rs, a_ss, a_rs, x_ss, x_rs,
    s_ss, s_rs, o_ss, o_rs, h_ss, h_rs, r_ss, r_rs,
):
    tok = q_ref.shape[0]
    tp = 4
    rown = tok // tp
    width = out_ref.shape[1]
    per = n // groups
    half_n = n // 2
    e = lax.axis_index("sp")
    j = lax.axis_index("tp")
    jx, jc = j // 2, j % 2
    xp = (1 - jx) * 2 + jc
    sib = jx * 2 + (1 - jc)
    a, b = e // 2, e % 2
    ypart = a * 2 + (1 - b)

    def rcopy(src, dst, ss, rs, s_id, t_id):
        return pltpu.make_async_remote_copy(
            src_ref=src, dst_ref=dst, send_sem=ss, recv_sem=rs,
            device_id=(s_id, t_id), device_id_type=MESH,
        )

    locals_ = [
        pltpu.make_async_copy(tab_h.at[pl.ds(e * tok, tok)], tab, loc.at[0]),
        pltpu.make_async_copy(dw_h.at[0], dw.at[j], loc.at[1]),
        pltpu.make_async_copy(ow_h, ow, loc.at[2]),
        pltpu.make_async_copy(resid_h, resid, loc.at[3]),
        pltpu.make_async_copy(gw_h.at[0], gw, loc.at[4]),
        pltpu.make_async_copy(uw_h.at[0], uw, loc.at[5]),
    ]
    for c in locals_:
        c.start()

    barrier = pltpu.get_barrier_semaphore()

    def greet(k, carry):
        pl.semaphore_signal(barrier, inc=1, device_id=(lax.rem(e + k, n), j), device_id_type=MESH)
        return carry

    lax.fori_loop(1, n, greet, 0)
    for k in range(1, tp):
        pl.semaphore_signal(barrier, inc=1, device_id=(e, lax.rem(j + k, tp)), device_id_type=MESH)

    locals_[0].wait()
    cs = tab[:, : HEAD_DIM // 2]
    sn = tab[:, HEAD_DIM // 2 :]
    cos4 = jnp.concatenate([cs, cs, cs, cs], axis=1)
    sin4 = jnp.concatenate([-sn, sn, -sn, sn], axis=1)
    low = lane_of((tok, LANES)) < HEAD_DIM
    kv_in = jnp.concatenate([k_ref[...].astype(F32), v_ref[...].astype(F32)], axis=0).T
    kgain = jnp.concatenate([kg_ref[...], kg_ref[...]], axis=1)
    kv[e] = jnp.where(low, prepare(kv_in, kgain, cos4, sin4), kv_in).astype(BF)
    pl.semaphore_wait(barrier, n - 1 + tp - 1)

    def kv_send(d):
        to = lax.rem(a + d, half_n) * 2 + b
        return rcopy(kv.at[e], kv.at[e], kv_ss.at[d], kv_rs.at[d], to, j)

    def kv_recv(d):
        src = lax.rem(a + half_n - d, half_n) * 2 + b
        return rcopy(kv.at[src], kv.at[src], kv_ss.at[d], kv_rs.at[d], e, j)

    def kf_send(d):
        src = lax.rem(a + half_n - d, half_n) * 2 + b
        return rcopy(kv.at[src], kv.at[src], kf_ss.at[d], kf_rs.at[d], ypart, j)

    def kf_recv(d):
        src = lax.rem(a + half_n - d, half_n) * 2 + (1 - b)
        return rcopy(kv.at[src], kv.at[src], kf_ss.at[d], kf_rs.at[d], ypart, j)

    def loop(lo, hi, fn):
        def step(i, carry):
            fn(i)
            return carry
        lax.fori_loop(lo, hi, step, 0)

    loop(1, half_n, lambda d: kv_send(d).start())
    kf_send(0).start()

    locals_[1].wait()
    ff = dw.shape[1]
    early = 3 * ff // 4

    def dw_x(part_id, owner):
        rows_of = pl.ds(0, early) if part_id == 0 else pl.ds(early, ff - early)
        sem = 3 * part_id
        return rcopy(dw.at[owner, rows_of], dw.at[owner, rows_of], dw_ss.at[sem], dw_rs.at[sem], e, xp)

    dw_s = rcopy(dw.at[j], dw.at[j], dw_ss.at[1], dw_rs.at[1], e, sib)
    dw_o = rcopy(dw.at[xp], dw.at[xp], dw_ss.at[2], dw_rs.at[2], e, sib)
    dw_x(0, j).start()
    dw_s.start()

    qgain = jnp.concatenate([qg_ref[0:1, :], qg_ref[1:2, :]], axis=1)
    q = prepare(q_ref[...].astype(F32), qgain, cos4, sin4) * (HEAD_DIM**-0.5)
    qx[0:tok] = jnp.where(low, q, 0.0).astype(BF)
    qx[tok : 2 * tok] = jnp.where(low, pltpu.roll(q, HEAD_DIM, 1), 0.0).astype(BF)
    mx[...] = jnp.full(mx.shape, -jnp.inf, F32)
    acc[...] = jnp.zeros(acc.shape, F32)

    def attend(d):
        @pl.when(d > 0)
        def _():
            kv_recv(d).wait_recv()
            kf_send(d).start()

        kf_recv(d).wait_recv()
        base = lax.rem(a + half_n - d, half_n) * 2
        keys = jnp.concatenate([kv[base], kv[base + 1]], axis=0)
        vals = jnp.where(lane_of(keys.shape) < HEAD_DIM, jnp.ones_like(keys), keys)
        for blk in range(4):
            rs = pl.ds(blk * (2 * tok // 4), 2 * tok // 4)
            sc = lax.dot_general(qx[rs], keys, (((1,), (1,)), ((), ())), preferred_element_type=F32)
            old = mx[rs]
            new = jnp.maximum(old, jnp.max(sc, axis=-1, keepdims=True))
            p = jnp.exp(sc - new[:, 0:1])
            mx[rs] = new
            acc[rs] = acc[rs] * jnp.exp(old - new) + jnp.dot(p.astype(BF), vals, preferred_element_type=F32)

    loop(0, half_n, attend)
    o = acc[...]
    o = o / pltpu.roll(o, HEAD_DIM, 1)
    att[...] = jnp.where(low, pltpu.roll(o[0:tok], HEAD_DIM, 1), o[tok : 2 * tok]).astype(BF)

    def at_copy(k):
        to = lax.rem(j + k, tp)
        return rcopy(att.at[pl.ds(to * rown, rown)], attg.at[j], at_ss.at[k], at_rs.at[k], e, to)

    def at_recv(k):
        src = lax.rem(j + tp - k, tp)
        return rcopy(att.at[pl.ds(0, rown)], attg.at[src], at_ss.at[k], at_rs.at[k], e, src)

    for k in range(1, tp):
        at_copy(k).start()
    dw_x(1, j).start()
    attg[j] = att[pl.ds(j * rown, rown), :]

    slots = n * cap
    ids_f = jnp.concatenate([ids_ref[...].astype(F32), jnp.zeros((6, tok), F32)], axis=0)
    ids_t[...] = ids_f.T
    ids = ids_t[pl.ds(j * rown, rown), :].astype(jnp.int32)
    rw = jnp.concatenate([rw_ref[...], jnp.zeros((6, rown), F32)], axis=0).T
    col = lax.broadcasted_iota(jnp.int32, (rown, slots), 1)
    off0 = col - ids[:, 0:1] * cap
    off1 = col - ids[:, 1:2] * cap
    in0 = (off0 >= 0) & (off0 < cap)
    in1 = (off1 >= 0) & (off1 < cap)
    member = jnp.where(in0 | in1, 1.0, 0.0)
    ti = lax.broadcasted_iota(jnp.int32, (rown, rown), 0)
    tj = lax.broadcasted_iota(jnp.int32, (rown, rown), 1)
    before = jnp.where(tj < ti, 1.0, 0.0)
    rank = jnp.dot(before.astype(BF), member.astype(BF), preferred_element_type=F32)
    offset = jnp.where(in0, off0, off1).astype(F32)
    hit = jnp.where(rank == offset, member, 0.0)
    weight = hit * jnp.where(in0, rw[:, 0:1], rw[:, 1:2])

    locals_[2].wait()
    locals_[3].wait()
    for k in range(1, tp):
        at_recv(k).wait_recv()
    joined = jnp.concatenate([attg[i] for i in range(tp)], axis=1)
    mixed = jnp.dot(joined, ow[...], preferred_element_type=F32)
    residual = (resid[...].astype(F32) + mixed).astype(BF).astype(F32)
    res_f[...] = residual
    scale = lax.rsqrt(jnp.mean(residual * residual, axis=-1, keepdims=True) + eps)
    normed = (residual * scale * ng_ref[...]).astype(BF)
    out_rows = lax.dot_general(
        hit.astype(BF), normed, (((0,), (0,)), ((), ())), preferred_element_type=F32
    )
    send[...] = out_rows.reshape(n, cap, width).astype(BF)

    def a_send(k):
        to = lax.rem(e + k, n)
        return rcopy(send.at[to], rows.at[j, k], a_ss.at[k], a_rs.at[k], to, j)

    def a_recv(k):
        return rcopy(send.at[0], rows.at[j, k], a_ss.at[k], a_rs.at[k], e, j)

    loop(1, n, lambda k: a_send(k).start())
    rows[j, 0] = send[e]
    locals_[4].wait()
    locals_[5].wait()

    def part(t, g):
        return rows.at[t, pl.ds(g * per, per)]

    def x_send(g):
        return rcopy(part(j, g), part(j, g), x_ss.at[g], x_rs.at[g], e, xp)

    def x_recv(g):
        return rcopy(part(xp, g), part(xp, g), x_ss.at[g], x_rs.at[g], e, xp)

    def s_send(g):
        return rcopy(part(j, g), part(j, g), s_ss.at[g], s_rs.at[g], e, sib)

    def s_recv(g):
        return rcopy(part(sib, g), part(sib, g), s_ss.at[g], s_rs.at[g], e, sib)

    def o_send(g):
        return rcopy(part(xp, g), part(xp, g), o_ss.at[g], o_rs.at[g], e, sib)

    dg = (1 - jx) * 2 + (1 - jc)

    def o_recv(g):
        return rcopy(part(dg, g), part(dg, g), o_ss.at[g], o_rs.at[g], e, sib)

    def h_send(g, k):
        to = lax.rem(j + k, tp)
        return rcopy(hid.at[g, to], hidg.at[g, j], h_ss.at[g, k], h_rs.at[g, k], e, to)

    def h_recv(g, k):
        src = lax.rem(j + tp - k, tp)
        return rcopy(hid.at[g, 0], hidg.at[g, src], h_ss.at[g, k], h_rs.at[g, k], e, src)

    def r_send(k):
        to = lax.rem(e + n - k, n)
        return rcopy(back.at[k], ret.at[e], r_ss.at[k], r_rs.at[k], to, j)

    def r_recv(k):
        src = lax.rem(e + k, n)
        return rcopy(back.at[k], ret.at[src], r_ss.at[k], r_rs.at[k], e, j)

    m = per * cap

    def stage_a(g):
        def one(i):
            k = g * per + i

            @pl.when(k > 0)
            def _():
                a_recv(k).wait_recv()

        loop(0, per, one)
        x_send(g).start()
        s_send(g).start()

    def stage_c(g):
        x_recv(g).wait_recv()
        o_send(g).start()

        @pl.when(g == 0)
        def _():
            dw_x(0, xp).wait_recv()
            dw_x(1, xp).wait_recv()
            dw_o.start()

        s_recv(g).wait_recv()
        o_recv(g).wait_recv()
        block = rows[:, pl.ds(g * per, per)].astype(F32).reshape(tp * m, width).astype(BF)
        gate = jnp.dot(block, gw[...], preferred_element_type=F32)
        upper = jnp.dot(block, uw[...], preferred_element_type=F32)
        hidden = gate / (1.0 + jnp.exp(-gate)) * upper
        hid[g] = hidden.reshape(tp, m, hidden.shape[1]).astype(BF)
        for k in range(1, tp):
            h_send(g, k).start()
        hidg[g, j] = hid[g, j]

    def stage_d(g):
        for k in range(1, tp):
            h_recv(g, k).wait_recv()

        @pl.when(g == 0)
        def _():
            rcopy(dw.at[sib], dw.at[sib], dw_ss.at[1], dw_rs.at[1], e, sib).wait_recv()
            rcopy(dw.at[dg], dw.at[dg], dw_ss.at[2], dw_rs.at[2], e, sib).wait_recv()

        joined_h = jnp.concatenate([hidg[g, i] for i in range(tp)], axis=1)
        cols = 512

        def column(ci):
            cd = pl.ds(pl.multiple_of(ci * cols, cols), cols)
            dfull = dw[:, :, cd].reshape(joined_h.shape[1], cols)
            y = jnp.dot(joined_h, dfull, preferred_element_type=F32)
            back[pl.ds(g * per, per), :, cd] = y.reshape(per, cap, cols).astype(BF)

        for ci in range(width // cols):
            column(ci)

        def one(i):
            k = g * per + i

            @pl.when(k > 0)
            def _():
                r_send(k).start()

        loop(0, per, one)

    def tick(t):
        @pl.when(t < groups)
        def _():
            stage_a(t)

        @pl.when(t >= 2)
        def _():
            stage_d(t - 2)

        @pl.when((t >= 1) & (t <= groups))
        def _():
            stage_c(t - 1)

    loop(0, groups + 2, tick)
    ret[e] = back[0]
    loop(1, n, lambda k: r_recv(k).wait_recv())
    w_hi = weight.astype(BF)
    w_lo = (weight - w_hi.astype(F32)).astype(BF)
    back_rows = ret[...].astype(F32).reshape(slots, width).astype(BF)
    total = jnp.dot(w_hi, back_rows, preferred_element_type=F32)
    total += jnp.dot(w_lo, back_rows, preferred_element_type=F32)
    out_ref[...] = (res_f[...] + total).astype(BF)

    def drain(k):
        a_send(k).wait_send()
        r_send(k).wait_send()

    loop(1, n, drain)
    loop(1, half_n, lambda d: kv_send(d).wait_send())
    loop(0, half_n, lambda d: kf_send(d).wait_send())
    for k in range(1, tp):
        at_copy(k).wait_send()
    dw_x(0, j).wait_send()
    dw_x(1, j).wait_send()
    dw_s.wait_send()
    dw_o.wait_send()

    def drain_g(g):
        x_send(g).wait_send()
        s_send(g).wait_send()
        o_send(g).wait_send()
        for k in range(1, tp):
            h_send(g, k).wait_send()

    loop(0, groups, drain_g)


def body(resid_in, query_proj, key_proj, value_proj, query_gain, key_gain, out_weight, norm_gain,
         gate_weight, up_weight, down_weight, expert_ids, route_weight):
    n = lax.axis_size("sp")
    tp = lax.axis_size("tp")
    tok = query_proj.shape[0]
    rown = tok // tp
    width = resid_in.shape[1]
    ff = gate_weight.shape[2]
    need = max(2, 3 * TOPK * TOK_DEV // (2 * tp * n))
    cap = -(-need // 8) * 8
    groups = min(4, n)
    per = n // groups
    table = jnp.asarray(rotary_table(n * tok))
    vm = pl.BlockSpec(memory_space=pltpu.VMEM)
    hb = pl.BlockSpec(memory_space=pl.ANY)
    dma = pltpu.SemaphoreType.DMA
    V = pltpu.VMEM
    scratch = [
        V((rown, width), BF),
        V(out_weight.shape, BF),
        V((width, ff), BF),
        V((width, ff), BF),
        V((tp, ff, width), BF),
        V((tok, HEAD_DIM), F32),
        V((n, tok, LANES), BF),
        V((2 * tok, LANES), BF),
        V((2 * tok, LANES), F32),
        V((2 * tok, LANES), F32),
        V((tok, LANES), BF),
        V((tp, rown, LANES), BF),
        V((rown, width), F32),
        V((n, cap, width), BF),
        V((tp, n, cap, width), BF),
        V((groups, tp, per * cap, ff), BF),
        V((groups, tp, per * cap, ff), BF),
        V((n, cap, width), BF),
        V((n, cap, width), BF),
        V((tok, 8), F32),
        dma((6,)),
        dma((n // 2,)), dma((n // 2,)), dma((n // 2,)), dma((n // 2,)),
        dma((tp,)), dma((tp,)), dma((4,)), dma((4,)),
        dma((n,)), dma((n,)),
        dma((groups,)), dma((groups,)), dma((groups,)), dma((groups,)), dma((groups,)), dma((groups,)),
        dma((groups, tp)), dma((groups, tp)),
        dma((n,)), dma((n,)),
    ]
    out = pl.pallas_call(
        functools.partial(kernel, n, cap, groups),
        out_shape=jax.ShapeDtypeStruct((rown, width), BF),
        in_specs=[hb, vm, vm, vm, vm, vm, hb, vm, hb, hb, hb, vm, vm, hb],
        out_specs=vm,
        scratch_shapes=scratch,
        compiler_params=pltpu.CompilerParams(
            collective_id=0, has_side_effects=True, vmem_limit_bytes=60 * 1024 * 1024
        ),
    )(resid_in, query_proj, key_proj.T, value_proj.T, query_gain, key_gain, out_weight,
      norm_gain.reshape(1, width), gate_weight, up_weight, down_weight, expert_ids.T, route_weight.T, table)
    return out


def solution(mesh):
    placed = (
        P(("sp", "tp"), None),
        P("sp", "tp"),
        P("sp", "tp"),
        P("sp", "tp"),
        P("tp", None),
        P("tp", None),
        P(),
        P(),
        P("sp", None, "tp"),
        P("sp", None, "tp"),
        P("sp", "tp", None),
        P("sp", None),
        P(("sp", "tp"), None),
    )
    return jax.shard_map(
        body, mesh=mesh, in_specs=placed, out_specs=P(("sp", "tp"), None), check_vma=False
    )
```

```python
import functools

import jax
import jax.numpy as jnp
import numpy as np
from jax import lax
from jax.experimental import pallas as pl
from jax.experimental.pallas import tpu as pltpu
from jax.sharding import PartitionSpec as P

HEAD_DIM = 64
TOPK = 2
GRID_W = 64
TOK_DEV = 256
LANES = 128

eps = 1e-06
rope_base = 10000.0

BF = jnp.bfloat16
F32 = jnp.float32
MESH = pl.DeviceIdType.MESH


def rotary_table(tokens):
    positions = np.arange(tokens)
    freq_count = HEAD_DIM // 4
    inverse = (rope_base ** (-np.arange(freq_count, dtype=np.float32) / freq_count)).astype(np.float32)
    row_pos = (positions // GRID_W).astype(np.float32)
    col_pos = (positions % GRID_W).astype(np.float32)
    angles = np.concatenate([row_pos[:, None] * inverse, col_pos[:, None] * inverse], axis=-1)
    angles = angles.astype(np.float32)
    return np.concatenate([np.cos(angles), np.sin(angles)], axis=-1).astype(np.float32)


def lane_of(shape):
    return lax.broadcasted_iota(jnp.int32, shape, 1)


def prepare(x, gain, cos4, sin4):
    lane = lane_of(x.shape)
    low = lane < HEAD_DIM
    sq = x * x
    s_low = jnp.sum(jnp.where(low, sq, 0.0), axis=-1, keepdims=True) / HEAD_DIM
    s_high = jnp.sum(jnp.where(low, 0.0, sq), axis=-1, keepdims=True) / HEAD_DIM
    y = x * jnp.where(low, lax.rsqrt(s_low + eps), lax.rsqrt(s_high + eps)) * gain
    half = HEAD_DIM // 2
    first = (lane % HEAD_DIM) < half
    swapped = jnp.where(first, pltpu.roll(y, LANES - half, 1), pltpu.roll(y, half, 1))
    return y * cos4 + swapped * sin4


def kernel(
    n, cap, groups,
    resid_h, q_ref, k_ref, v_ref, qg_ref, kg_ref, ow_h, ng_ref, gw_h, uw_h, dw_h, ids_ref, rw_ref, tab_h,
    out_ref,
    resid, ow, gw, uw, dw, tab, kv, qx, mx, acc, att, attg, res_f, send, rows, hid, hidg, back, ret, ids_t,
    loc, kv_ss, kv_rs, kf_ss, kf_rs, at_ss, at_rs, dw_ss, dw_rs, a_ss, a_rs, x_ss, x_rs,
    s_ss, s_rs, o_ss, o_rs, h_ss, h_rs, r_ss, r_rs,
):
    tok = q_ref.shape[0]
    tp = 4
    rown = tok // tp
    width = out_ref.shape[1]
    per = n // groups
    half_n = n // 2
    e = lax.axis_index("sp")
    j = lax.axis_index("tp")
    jx, jc = j // 2, j % 2
    xp = (1 - jx) * 2 + jc
    sib = jx * 2 + (1 - jc)
    a, b = e // 2, e % 2
    ypart = a * 2 + (1 - b)

    def rcopy(src, dst, ss, rs, s_id, t_id):
        return pltpu.make_async_remote_copy(
            src_ref=src, dst_ref=dst, send_sem=ss, recv_sem=rs,
            device_id=(s_id, t_id), device_id_type=MESH,
        )

    locals_ = [
        pltpu.make_async_copy(tab_h.at[pl.ds(e * tok, tok)], tab, loc.at[0]),
        pltpu.make_async_copy(dw_h.at[0], dw.at[j], loc.at[1]),
        pltpu.make_async_copy(ow_h, ow, loc.at[2]),
        pltpu.make_async_copy(resid_h, resid, loc.at[3]),
        pltpu.make_async_copy(gw_h.at[0], gw, loc.at[4]),
        pltpu.make_async_copy(uw_h.at[0], uw, loc.at[5]),
    ]
    for c in locals_:
        c.start()

    barrier = pltpu.get_barrier_semaphore()

    def greet(k, carry):
        pl.semaphore_signal(barrier, inc=1, device_id=(lax.rem(e + k, n), j), device_id_type=MESH)
        return carry

    lax.fori_loop(1, n, greet, 0)
    for k in range(1, tp):
        pl.semaphore_signal(barrier, inc=1, device_id=(e, lax.rem(j + k, tp)), device_id_type=MESH)

    locals_[0].wait()
    cs = tab[:, : HEAD_DIM // 2]
    sn = tab[:, HEAD_DIM // 2 :]
    cos4 = jnp.concatenate([cs, cs, cs, cs], axis=1)
    sin4 = jnp.concatenate([-sn, sn, -sn, sn], axis=1)
    low = lane_of((tok, LANES)) < HEAD_DIM
    kv_in = jnp.concatenate([k_ref[...].astype(F32), v_ref[...].astype(F32)], axis=0).T
    kgain = jnp.concatenate([kg_ref[...], kg_ref[...]], axis=1)
    kv[e] = jnp.where(low, prepare(kv_in, kgain, cos4, sin4), kv_in).astype(BF)
    qgain = jnp.concatenate([qg_ref[0:1, :], qg_ref[1:2, :]], axis=1)
    q = prepare(q_ref[...].astype(F32), qgain, cos4, sin4) * (HEAD_DIM**-0.5)
    qx[0:tok] = jnp.where(low, q, 0.0).astype(BF)
    qx[tok : 2 * tok] = jnp.where(low, pltpu.roll(q, HEAD_DIM, 1), 0.0).astype(BF)
    mx[...] = jnp.full(mx.shape, -jnp.inf, F32)
    acc[...] = jnp.zeros(acc.shape, F32)

    pl.semaphore_wait(barrier, n - 1 + tp - 1)

    def kv_send(d):
        to = lax.rem(a + d, half_n) * 2 + b
        return rcopy(kv.at[e], kv.at[e], kv_ss.at[d], kv_rs.at[d], to, j)

    def kv_recv(d):
        src = lax.rem(a + half_n - d, half_n) * 2 + b
        return rcopy(kv.at[src], kv.at[src], kv_ss.at[d], kv_rs.at[d], e, j)

    def kf_send(d):
        src = lax.rem(a + half_n - d, half_n) * 2 + b
        return rcopy(kv.at[src], kv.at[src], kf_ss.at[d], kf_rs.at[d], ypart, j)

    def kf_recv(d):
        src = lax.rem(a + half_n - d, half_n) * 2 + (1 - b)
        return rcopy(kv.at[src], kv.at[src], kf_ss.at[d], kf_rs.at[d], ypart, j)

    def loop(lo, hi, fn):
        def step(i, carry):
            fn(i)
            return carry
        lax.fori_loop(lo, hi, step, 0)

    loop(1, half_n, lambda d: kv_send(d).start())
    kf_send(0).start()

    locals_[1].wait()
    ff = dw.shape[1]
    early = 3 * ff // 4

    def dw_x(part_id, owner):
        rows_of = pl.ds(0, early) if part_id == 0 else pl.ds(early, ff - early)
        sem = 3 * part_id
        return rcopy(dw.at[owner, rows_of], dw.at[owner, rows_of], dw_ss.at[sem], dw_rs.at[sem], e, xp)

    dw_s = rcopy(dw.at[j], dw.at[j], dw_ss.at[1], dw_rs.at[1], e, sib)
    dw_o = rcopy(dw.at[xp], dw.at[xp], dw_ss.at[2], dw_rs.at[2], e, sib)
    dw_x(0, j).start()
    dw_s.start()

    def attend(d):
        @pl.when(d > 0)
        def _():
            kv_recv(d).wait_recv()
            kf_send(d).start()

        kf_recv(d).wait_recv()
        base = lax.rem(a + half_n - d, half_n) * 2
        keys = jnp.concatenate([kv[base], kv[base + 1]], axis=0)
        vals = jnp.where(lane_of(keys.shape) < HEAD_DIM, jnp.ones_like(keys), keys)
        for blk in range(4):
            rs = pl.ds(blk * (2 * tok // 4), 2 * tok // 4)
            sc = lax.dot_general(qx[rs], keys, (((1,), (1,)), ((), ())), preferred_element_type=F32)
            old = mx[rs]
            new = jnp.maximum(old, jnp.max(sc, axis=-1, keepdims=True))
            p = jnp.exp(sc - new[:, 0:1])
            mx[rs] = new
            acc[rs] = acc[rs] * jnp.exp(old - new) + jnp.dot(p.astype(BF), vals, preferred_element_type=F32)

    slots = n * cap
    ids_f = jnp.concatenate([ids_ref[...].astype(F32), jnp.zeros((6, tok), F32)], axis=0)
    ids_t[...] = ids_f.T
    ids = ids_t[pl.ds(j * rown, rown), :].astype(jnp.int32)
    rw = jnp.concatenate([rw_ref[...], jnp.zeros((6, rown), F32)], axis=0).T
    col = lax.broadcasted_iota(jnp.int32, (rown, slots), 1)
    off0 = col - ids[:, 0:1] * cap
    off1 = col - ids[:, 1:2] * cap
    in0 = (off0 >= 0) & (off0 < cap)
    in1 = (off1 >= 0) & (off1 < cap)
    member = jnp.where(in0 | in1, 1.0, 0.0)
    ti = lax.broadcasted_iota(jnp.int32, (rown, rown), 0)
    tj = lax.broadcasted_iota(jnp.int32, (rown, rown), 1)
    before = jnp.where(tj < ti, 1.0, 0.0)
    rank = jnp.dot(before.astype(BF), member.astype(BF), preferred_element_type=F32)
    offset = jnp.where(in0, off0, off1).astype(F32)
    hit = jnp.where(rank == offset, member, 0.0)
    weight = hit * jnp.where(in0, rw[:, 0:1], rw[:, 1:2])

    loop(0, half_n, attend)
    o = acc[...]
    o = o / pltpu.roll(o, HEAD_DIM, 1)
    att[...] = jnp.where(low, pltpu.roll(o[0:tok], HEAD_DIM, 1), o[tok : 2 * tok]).astype(BF)

    def at_copy(k):
        to = lax.rem(j + k, tp)
        return rcopy(att.at[pl.ds(to * rown, rown)], attg.at[j], at_ss.at[k], at_rs.at[k], e, to)

    def at_recv(k):
        src = lax.rem(j + tp - k, tp)
        return rcopy(att.at[pl.ds(0, rown)], attg.at[src], at_ss.at[k], at_rs.at[k], e, src)

    for k in range(1, tp):
        at_copy(k).start()
    dw_x(1, j).start()
    attg[j] = att[pl.ds(j * rown, rown), :]

    locals_[2].wait()
    locals_[3].wait()
    for k in range(1, tp):
        at_recv(k).wait_recv()
    joined = jnp.concatenate([attg[i] for i in range(tp)], axis=1)
    mixed = jnp.dot(joined, ow[...], preferred_element_type=F32)
    residual = (resid[...].astype(F32) + mixed).astype(BF).astype(F32)
    res_f[...] = residual
    scale = lax.rsqrt(jnp.mean(residual * residual, axis=-1, keepdims=True) + eps)
    normed = (residual * scale * ng_ref[...]).astype(BF)
    out_rows = lax.dot_general(
        hit.astype(BF), normed, (((0,), (0,)), ((), ())), preferred_element_type=F32
    )
    send[...] = out_rows.reshape(n, cap, width).astype(BF)

    def split(i):
        p = i // 2
        q = ((p + half_n - 1) // half_n) * (1 + p % (half_n - 1))
        return q // 2, q % 2, i % 2

    def target(i):
        k0, k1, kb = split(i)
        return ((a // 2 + k0) % (half_n // 2)) * 4 + ((a % 2 + k1) % 2) * 2 + (b + kb) % 2

    def source(i):
        k0, k1, kb = split(i)
        return ((a // 2 + half_n // 2 - k0) % (half_n // 2)) * 4 + ((a % 2 + k1) % 2) * 2 + (b + kb) % 2

    def a_send(k):
        to = target(k)
        return rcopy(send.at[to], rows.at[j, k], a_ss.at[k], a_rs.at[k], to, j)

    def a_recv(k):
        return rcopy(send.at[0], rows.at[j, k], a_ss.at[k], a_rs.at[k], e, j)

    loop(1, n, lambda k: a_send(k).start())
    rows[j, 0] = send[e]
    locals_[4].wait()
    locals_[5].wait()

    def part(t, g):
        return rows.at[t, pl.ds(g * per, per)]

    def x_send(g):
        return rcopy(part(j, g), part(j, g), x_ss.at[g], x_rs.at[g], e, xp)

    def x_recv(g):
        return rcopy(part(xp, g), part(xp, g), x_ss.at[g], x_rs.at[g], e, xp)

    def s_send(g):
        return rcopy(part(j, g), part(j, g), s_ss.at[g], s_rs.at[g], e, sib)

    def s_recv(g):
        return rcopy(part(sib, g), part(sib, g), s_ss.at[g], s_rs.at[g], e, sib)

    def o_send(g):
        return rcopy(part(xp, g), part(xp, g), o_ss.at[g], o_rs.at[g], e, sib)

    dg = (1 - jx) * 2 + (1 - jc)

    def o_recv(g):
        return rcopy(part(dg, g), part(dg, g), o_ss.at[g], o_rs.at[g], e, sib)

    def h_send(g, k):
        to = lax.rem(j + k, tp)
        return rcopy(hid.at[g, to], hidg.at[g, j], h_ss.at[g, k], h_rs.at[g, k], e, to)

    def h_recv(g, k):
        src = lax.rem(j + tp - k, tp)
        return rcopy(hid.at[g, 0], hidg.at[g, src], h_ss.at[g, k], h_rs.at[g, k], e, src)

    def r_send(k):
        to = source(k)
        return rcopy(back.at[k], ret.at[e], r_ss.at[k], r_rs.at[k], to, j)

    def r_recv(k):
        src = target(k)
        return rcopy(back.at[k], ret.at[src], r_ss.at[k], r_rs.at[k], e, j)

    m = per * cap

    def stage_a(g):
        def one(i):
            k = g * per + i

            @pl.when(k > 0)
            def _():
                a_recv(k).wait_recv()

        loop(0, per, one)
        x_send(g).start()
        s_send(g).start()

    def stage_c(g):
        x_recv(g).wait_recv()
        o_send(g).start()

        @pl.when(g == 0)
        def _():
            dw_x(0, xp).wait_recv()
            dw_x(1, xp).wait_recv()
            dw_o.start()

        s_recv(g).wait_recv()
        o_recv(g).wait_recv()
        block = rows[:, pl.ds(g * per, per)].astype(F32).reshape(tp * m, width).astype(BF)
        gate = jnp.dot(block, gw[...], preferred_element_type=F32)
        upper = jnp.dot(block, uw[...], preferred_element_type=F32)
        hidden = gate / (1.0 + jnp.exp(-gate)) * upper
        hid[g] = hidden.reshape(tp, m, hidden.shape[1]).astype(BF)
        for k in range(1, tp):
            h_send(g, k).start()
        hidg[g, j] = hid[g, j]

    def stage_d(g):
        for k in range(1, tp):
            h_recv(g, k).wait_recv()

        @pl.when(g == 0)
        def _():
            rcopy(dw.at[sib], dw.at[sib], dw_ss.at[1], dw_rs.at[1], e, sib).wait_recv()
            rcopy(dw.at[dg], dw.at[dg], dw_ss.at[2], dw_rs.at[2], e, sib).wait_recv()

        joined_h = jnp.concatenate([hidg[g, i] for i in range(tp)], axis=1)
        cols = 512

        def column(ci):
            cd = pl.ds(pl.multiple_of(ci * cols, cols), cols)
            dfull = dw[:, :, cd].reshape(joined_h.shape[1], cols)
            y = jnp.dot(joined_h, dfull, preferred_element_type=F32)
            back[pl.ds(g * per, per), :, cd] = y.reshape(per, cap, cols).astype(BF)

        for ci in range(width // cols):
            column(ci)

        def one(i):
            k = g * per + i

            @pl.when(k > 0)
            def _():
                r_send(k).start()

        loop(0, per, one)

    def tick(t):
        @pl.when(t < groups)
        def _():
            stage_a(t)

        @pl.when(t >= 2)
        def _():
            stage_d(t - 2)

        @pl.when((t >= 1) & (t <= groups))
        def _():
            stage_c(t - 1)

    loop(0, groups + 2, tick)
    ret[e] = back[0]
    loop(1, n, lambda k: r_recv(k).wait_recv())
    w_hi = weight.astype(BF)
    w_lo = (weight - w_hi.astype(F32)).astype(BF)
    back_rows = ret[...].astype(F32).reshape(slots, width).astype(BF)
    total = jnp.dot(w_hi, back_rows, preferred_element_type=F32)
    total += jnp.dot(w_lo, back_rows, preferred_element_type=F32)
    out_ref[...] = (res_f[...] + total).astype(BF)

    def drain(k):
        a_send(k).wait_send()
        r_send(k).wait_send()

    loop(1, n, drain)
    loop(1, half_n, lambda d: kv_send(d).wait_send())
    loop(0, half_n, lambda d: kf_send(d).wait_send())
    for k in range(1, tp):
        at_copy(k).wait_send()
    dw_x(0, j).wait_send()
    dw_x(1, j).wait_send()
    dw_s.wait_send()
    dw_o.wait_send()

    def drain_g(g):
        x_send(g).wait_send()
        s_send(g).wait_send()
        o_send(g).wait_send()
        for k in range(1, tp):
            h_send(g, k).wait_send()

    loop(0, groups, drain_g)


def body(resid_in, query_proj, key_proj, value_proj, query_gain, key_gain, out_weight, norm_gain,
         gate_weight, up_weight, down_weight, expert_ids, route_weight):
    n = lax.axis_size("sp")
    tp = lax.axis_size("tp")
    tok = query_proj.shape[0]
    rown = tok // tp
    width = resid_in.shape[1]
    ff = gate_weight.shape[2]
    need = max(2, 3 * TOPK * TOK_DEV // (2 * tp * n))
    cap = -(-need // 8) * 8
    groups = min(4, n)
    per = n // groups
    table = jnp.asarray(rotary_table(n * tok))
    vm = pl.BlockSpec(memory_space=pltpu.VMEM)
    hb = pl.BlockSpec(memory_space=pl.ANY)
    dma = pltpu.SemaphoreType.DMA
    V = pltpu.VMEM
    scratch = [
        V((rown, width), BF),
        V(out_weight.shape, BF),
        V((width, ff), BF),
        V((width, ff), BF),
        V((tp, ff, width), BF),
        V((tok, HEAD_DIM), F32),
        V((n, tok, LANES), BF),
        V((2 * tok, LANES), BF),
        V((2 * tok, LANES), F32),
        V((2 * tok, LANES), F32),
        V((tok, LANES), BF),
        V((tp, rown, LANES), BF),
        V((rown, width), F32),
        V((n, cap, width), BF),
        V((tp, n, cap, width), BF),
        V((groups, tp, per * cap, ff), BF),
        V((groups, tp, per * cap, ff), BF),
        V((n, cap, width), BF),
        V((n, cap, width), BF),
        V((tok, 8), F32),
        dma((6,)),
        dma((n // 2,)), dma((n // 2,)), dma((n // 2,)), dma((n // 2,)),
        dma((tp,)), dma((tp,)), dma((4,)), dma((4,)),
        dma((n,)), dma((n,)),
        dma((groups,)), dma((groups,)), dma((groups,)), dma((groups,)), dma((groups,)), dma((groups,)),
        dma((groups, tp)), dma((groups, tp)),
        dma((n,)), dma((n,)),
    ]
    out = pl.pallas_call(
        functools.partial(kernel, n, cap, groups),
        out_shape=jax.ShapeDtypeStruct((rown, width), BF),
        in_specs=[hb, vm, vm, vm, vm, vm, hb, vm, hb, hb, hb, vm, vm, hb],
        out_specs=vm,
        scratch_shapes=scratch,
        compiler_params=pltpu.CompilerParams(
            collective_id=0, has_side_effects=True, vmem_limit_bytes=60 * 1024 * 1024
        ),
    )(resid_in, query_proj, key_proj.T, value_proj.T, query_gain, key_gain, out_weight,
      norm_gain.reshape(1, width), gate_weight, up_weight, down_weight, expert_ids.T, route_weight.T, table)
    return out


def solution(mesh):
    placed = (
        P(("sp", "tp"), None),
        P("sp", "tp"),
        P("sp", "tp"),
        P("sp", "tp"),
        P("tp", None),
        P("tp", None),
        P(),
        P(),
        P("sp", None, "tp"),
        P("sp", None, "tp"),
        P("sp", "tp", None),
        P("sp", None),
        P(("sp", "tp"), None),
    )
    return jax.shard_map(
        body, mesh=mesh, in_specs=placed, out_specs=P(("sp", "tp"), None), check_vma=False
    )
```
